32 devices in a mesh: sp: 8 (over z, x), tp: 4 (over y, core).
Axes of the slice: x: 2, y: 2, z: 4, core: 2. Of those that a mesh axis runs over, the one named last changes fastest.
Arguments:
- query_rows: bfloat16 [8192, 1024], P('sp', 'tp'), may hold values from -8 to 8
- key_rows: bfloat16 [8192, 1024], P('sp', 'tp'), may hold values from -8 to 8
- value_rows: bfloat16 [8192, 1024], P('sp', 'tp'), may hold values from -6 to 6
- forget_cum: float32 [16, 8192], P('tp', 'sp'), may hold values from -8192 to 0, as said below
- doc_ids: int32 [8192], P('sp'), may hold values from 0 to 3, never falling along the last dimension, each value on 1 to 3072 neighbouring positions
- residual: bfloat16 [8192, 2048], P(('sp', 'tp')), may hold values from -6 to 6
- out_weight: bfloat16 [1024, 2048], replicated, may hold values from -1.5 to 1.5
- norm_gain: float32 [2048], replicated, may hold values from 0.1 to 1.9
- expert_ids: int32 [8192, 2], P(('sp', 'tp')), may hold values from 0 to 7, as said below
- route_weights: float32 [8192, 2], P(('sp', 'tp')), may hold values from 0.2 to 1
- gate_proj: bfloat16 [8, 2048, 512], P('sp'), may hold values from -0.125 to 0.125
- up_proj: bfloat16 [8, 2048, 512], P('sp'), may hold values from -0.125 to 0.125
- down_proj: bfloat16 [8, 512, 2048], P('sp'), may hold values from -0.25 to 0.25
Outputs:
- layer_out: bfloat16 [8192, 2048], P(('sp', 'tp'))
The draws below stay inside these ranges and needn't reach their ends.
Inputs may be any that keep to these rules, and one draw needn't show every extreme that they name: `forget_cum`: each head's values never rise along the positions. `doc_ids`: document numbers never fall along the positions; a document holds at most 3072 positions, and one holds exactly 3072. `expert_ids`: a token's 2 experts differ and lie in one group of 4 consecutive experts; among the 256 rows of one device no expert is named more than 160 times, and in every draw one expert is named exactly 160 times by the rows of every device.
All inputs are finite; a program needn't handle non-finite values.
Results may differ from the reference program's by a relative error of at most 0.0054.
Values may be sent and summed in bfloat16 or wider, within the bound.
A program may use at most 128 MiB of HBM per device.

```python
import math
import jax
import jax.numpy as jnp
import numpy as np
from jax import lax

D = 2048
HEAD_COUNT = 16
HD = 64
FFE = 512
EPG = 4
TOPK = 2
REACH = 3
TOK_DEV = 1024
TOKEN_COUNT = 8192
TOK_LOC = 256
MOST = 3072
DOCS = 4
EXPERTS = 8
GROUPS = 2
CAP = 160


def draw_query_rows(key, part):
    width = HEAD_COUNT * HD
    base = jnp.clip(jax.random.normal(jax.random.fold_in(key, 1), (TOKEN_COUNT, width), jnp.float32), -6.0, 6.0)
    return base.astype(jnp.bfloat16)


def draw_key_rows(key, part):
    width = HEAD_COUNT * HD
    base = jnp.clip(jax.random.normal(jax.random.fold_in(key, 3), (TOKEN_COUNT, width), jnp.float32), -6.0, 6.0)
    return base.astype(jnp.bfloat16)


def draw_forget_cum(key, part):
    order = jax.random.permutation(jax.random.fold_in(key, 5), HEAD_COUNT)
    fast_count = HEAD_COUNT // 2
    quick_route = order < fast_count
    fast_rate = jnp.exp(jax.random.uniform(jax.random.fold_in(key, 6), (HEAD_COUNT,), jnp.float32, jnp.log(1.0 / 100.0), jnp.log(1.0 / 30.0)))
    slow_rate = jnp.exp(jax.random.uniform(jax.random.fold_in(key, 7), (HEAD_COUNT,), jnp.float32, jnp.log(0.3), jnp.log(1.0))) / TOKEN_COUNT
    rate = jnp.where(quick_route, fast_rate, slow_rate)
    device_factor = jnp.exp(jax.random.uniform(jax.random.fold_in(key, 8), (HEAD_COUNT, TOKEN_COUNT // TOK_DEV), jnp.float32, jnp.log(0.5), jnp.log(2.0)))
    device_factor = jnp.repeat(device_factor, TOK_DEV, axis=1)
    rough = jax.random.uniform(jax.random.fold_in(key, 9), (HEAD_COUNT, TOKEN_COUNT), jnp.float32, 0.0, 2.0)
    gate_logarithm = -rate[:, None] * device_factor * rough
    spike_positions = jax.random.randint(jax.random.fold_in(key, 10), (HEAD_COUNT, 2), 0, TOKEN_COUNT)
    spike_loss = jax.random.uniform(jax.random.fold_in(key, 11), (HEAD_COUNT, 2), jnp.float32, jnp.log(0.5), jnp.log(0.8))
    target_locations = jnp.arange(TOKEN_COUNT, dtype=jnp.int32)
    match_counts = target_locations[None, None, :] == spike_positions[:, :, None]
    spike_events = jnp.sum(jnp.where(match_counts, spike_loss[:, :, None], 0.0), axis=1)
    gate_logarithm = gate_logarithm + jnp.where(quick_route[:, None], 0.0, spike_events)
    return jnp.cumsum(gate_logarithm, axis=1).astype(jnp.float32)


def draw_expert_ids(key, part):
    block_total = TOKEN_COUNT // TOK_LOC
    busy_group = jax.random.randint(jax.random.fold_in(key, 12), (), 0, GROUPS)
    busy_local = jax.random.randint(jax.random.fold_in(key, 13), (), 0, EPG)

    def one_block(block_key):
        others = jnp.arange((GROUPS - 1) * CAP, dtype=jnp.int32) // CAP
        others = others + (others >= busy_group).astype(jnp.int32)
        chosen = jax.random.permutation(jax.random.fold_in(block_key, 1), others)[:TOK_LOC - CAP]
        groups = jnp.concatenate([jnp.full((CAP,), busy_group, jnp.int32), chosen.astype(jnp.int32)])
        groups = jax.random.permutation(jax.random.fold_in(block_key, 2), groups)
        first = jax.random.randint(jax.random.fold_in(block_key, 3), (TOK_LOC,), 0, EPG)
        first = jnp.where(groups == busy_group, busy_local, first)
        second = (first + jax.random.randint(jax.random.fold_in(block_key, 4), (TOK_LOC,), 1, EPG)) % EPG
        swap = jax.random.randint(jax.random.fold_in(block_key, 5), (TOK_LOC,), 0, 2)
        lower = jnp.where(swap == 1, second, first)
        upper = jnp.where(swap == 1, first, second)
        return jnp.stack([groups * EPG + lower, groups * EPG + upper], axis=1).astype(jnp.int32)
    block_keys = jax.random.split(jax.random.fold_in(key, 14), block_total)
    return jax.vmap(one_block)(block_keys).reshape(TOKEN_COUNT, TOPK).astype(jnp.int32)


def shard_levels(stream_key, shape, cuts, least, largest):
    def one(position, blocks):
        draws = jax.random.uniform(jax.random.fold_in(jax.random.fold_in(stream_key, 6), position), (blocks,), jnp.float32, least / len(cuts), largest / len(cuts))
        return jnp.repeat(jnp.exp(draws), shape[position] // blocks).reshape((-1,) + (1,) * (len(shape) - position - 1))

    gain = one(*cuts[0])
    for cut in cuts[1:]:
        gain = gain * one(*cut)
    return gain


def split_up(amount, total, reach, slope):
    loads = [(1 << 20) // math.isqrt(standing ** slope) + 1 for standing in range(2, amount + 1)]
    rest, given = total - reach - (amount - 1), [1] * (amount - 1)
    while rest > 0:
        candidates = [i for i in range(amount - 1) if given[i] < reach]
        mass, left = sum([loads[i] for i in candidates]), rest
        for i in candidates:
            addition = min(reach - given[i], max(1, left * loads[i] // mass), rest)
            given[i] = given[i] + addition
            rest = rest - addition
    return np.array([reach] + given)


def ragged(key, count, total, limit, slope):
    if count == 2:
        one = jax.random.randint(key, (), max(1, total - limit), min(limit, total - 1) + 1)
        return jnp.stack([one, total - one])
    tallies = jnp.asarray(split_up(count, total, limit, slope), jnp.int32)
    pairs = (count - 1) // 2
    source_of, taker = tallies[1:1 + 2 * pairs:2], tallies[2:2 + 2 * pairs:2]
    slack = jnp.minimum(source_of - 1, limit - taker)
    moved = jax.random.randint(jax.random.fold_in(key, 1), (pairs,), 0, 1 << 20) % (slack + 1)
    tallies = tallies.at[1:1 + 2 * pairs:2].set(source_of - moved).at[2:2 + 2 * pairs:2].set(taker + moved)
    return tallies[jax.random.permutation(jax.random.fold_in(key, 2), count)]


def bell_draw(rng, shape, deviation, bound, pieces=(), kind=jnp.bfloat16):
    drawn = jax.random.normal(rng, shape, jnp.float32) * deviation
    if len(pieces) > 0:
        drawn = shard_levels(rng, shape, pieces, -0.22, 0.18) * drawn
    return jnp.clip(drawn, min=-bound, max=bound).astype(kind)


def setup_inputs(seed: int = 0) -> dict:
    key_of = jax.random.split(jax.random.key(seed), 14)
    query_rows = draw_query_rows(jax.random.fold_in(key_of[13], 71), 0)
    key_rows = draw_key_rows(jax.random.fold_in(key_of[13], 71), 0)
    value_rows = bell_draw(key_of[2], (TOKEN_COUNT, HEAD_COUNT * HD), 1.0, 6.0, ((0, 8), (1, 4)))
    forget_cum = draw_forget_cum(jax.random.fold_in(key_of[13], 71), 0)
    doc_ids = jnp.searchsorted(jnp.cumsum(ragged(key_of[4], DOCS, TOKEN_COUNT, MOST, 2)), jnp.arange(TOKEN_COUNT), side="right").astype(jnp.int32)
    residual = bell_draw(key_of[5], (TOKEN_COUNT, D), 1.0, 6.0, ((0, 32),))
    out_weight = bell_draw(key_of[6], (HEAD_COUNT * HD, D), HEAD_COUNT ** -0.5, 1.5)
    norm_gain = jnp.clip(1.0 + 0.18 * jax.random.normal(key_of[7], (D,), jnp.float32), 0.1, 1.9)
    expert_ids = draw_expert_ids(jax.random.fold_in(key_of[13], 71), 0)
    route_weights = jnp.clip(0.2 + 0.8 * jax.random.uniform(key_of[9], (TOKEN_COUNT, TOPK), jnp.float32) ** shard_levels(key_of[9], (TOKEN_COUNT, TOPK), ((0, 32),), -0.2, 0.2), 0.2, 1.0)
    gate_proj = bell_draw(key_of[10], (EXPERTS, D, FFE), D ** -0.5, 0.125, ((0, 8),))
    up_proj = bell_draw(key_of[11], (EXPERTS, D, FFE), D ** -0.5, 0.125, ((0, 8),))
    down_proj = bell_draw(key_of[12], (EXPERTS, FFE, D), FFE ** -0.5, 0.25, ((0, 8),))
    return dict(query_rows=query_rows, key_rows=key_rows, value_rows=value_rows, forget_cum=forget_cum, doc_ids=doc_ids, residual=residual, out_weight=out_weight, norm_gain=norm_gain, expert_ids=expert_ids, route_weights=route_weights, gate_proj=gate_proj, up_proj=up_proj, down_proj=down_proj)


norm_eps = 1e-06
row_block = 128

def attention(query_rows, key_rows, value_rows, forget_cum, doc_ids):
    width = HEAD_COUNT * HD
    back = REACH * TOK_DEV
    span = back + TOK_DEV
    keys_pad = jnp.concatenate([jnp.zeros((back, width), jnp.bfloat16), key_rows], axis=0)
    values_pad = jnp.concatenate([jnp.zeros((back, width), jnp.bfloat16), value_rows], axis=0)
    gates_pad = jnp.concatenate([jnp.zeros((HEAD_COUNT, back), jnp.float32), forget_cum], axis=1)
    docs_pad = jnp.concatenate([jnp.full((back,), -1, jnp.int32), doc_ids.astype(jnp.int32)], axis=0)
    scale = HD ** (-0.5)

    def attend_block(index):
        start = (index * TOK_DEV).astype(jnp.int32)
        query = lax.dynamic_slice_in_dim(query_rows, start, TOK_DEV, 0).reshape(TOK_DEV, HEAD_COUNT, HD).astype(jnp.float32)
        keys = lax.dynamic_slice_in_dim(keys_pad, start, span, 0).reshape(span, HEAD_COUNT, HD).astype(jnp.float32)
        values = lax.dynamic_slice_in_dim(values_pad, start, span, 0).reshape(span, HEAD_COUNT, HD).astype(jnp.float32)
        query_gate = lax.dynamic_slice_in_dim(forget_cum, start, TOK_DEV, 1)
        key_gate = lax.dynamic_slice_in_dim(gates_pad, start, span, 1)
        query_doc = lax.dynamic_slice_in_dim(doc_ids.astype(jnp.int32), start, TOK_DEV, 0)
        key_doc = lax.dynamic_slice_in_dim(docs_pad, start, span, 0)
        score = jnp.einsum('thd,uhd->htu', query, keys) * scale
        score = score + query_gate[:, :, None] - key_gate[:, None, :]
        query_pos = start + jnp.arange(TOK_DEV, dtype=jnp.int32)
        key_pos = start - back + jnp.arange(span, dtype=jnp.int32)
        allowed = (key_pos[None, :] <= query_pos[:, None]) & (key_doc[None, :] == query_doc[:, None])
        score = jnp.where(allowed[None], score, -jnp.inf)
        top = lax.optimization_barrier(jnp.max(score, axis=-1))
        expo = jnp.exp(score - top[..., None])
        total = lax.optimization_barrier(jnp.sum(expo, axis=-1))
        rounded = lax.optimization_barrier(expo.astype(jnp.bfloat16)).astype(jnp.float32)
        summed = jnp.einsum('htu,uhd->thd', rounded, values)
        result = summed / jnp.transpose(total)[:, :, None]
        return result.astype(jnp.bfloat16).reshape(TOK_DEV, width)
    blocks = lax.map(attend_block, jnp.arange(TOKEN_COUNT // TOK_DEV, dtype=jnp.int32))
    return blocks.reshape(TOKEN_COUNT, width)

def experts_layer(normed, expert_ids, route_weights, gate_proj, up_proj, down_proj):
    assign = TOKEN_COUNT * TOPK
    flat_expert = expert_ids.reshape(assign).astype(jnp.int32)
    flat_token = (jnp.arange(assign, dtype=jnp.int32) // TOPK).astype(jnp.int32)
    flat_weight = route_weights.reshape(assign)
    order = jnp.argsort(flat_expert, stable=True)
    sorted_expert = flat_expert[order]
    sorted_token = flat_token[order]
    sorted_weight = flat_weight[order]
    counts = jnp.bincount(flat_expert, length=EXPERTS).astype(jnp.int32)
    padded = (counts + row_block - 1) // row_block * row_block
    start = jnp.cumsum(counts) - counts
    pad_end = jnp.cumsum(padded)
    pad_start = pad_end - padded
    dest = (pad_start[sorted_expert] + jnp.arange(assign, dtype=jnp.int32) - start[sorted_expert]).astype(jnp.int32)
    block_count = (assign + EXPERTS * (row_block - 1) + row_block - 1) // row_block
    buffer = jnp.zeros((block_count * row_block, D), jnp.bfloat16).at[dest].set(normed[sorted_token])
    block_expert = jnp.clip(jnp.searchsorted(pad_end, jnp.arange(block_count, dtype=jnp.int32) * row_block, side='right'), 0, EXPERTS - 1).astype(jnp.int32)

    def run_block(args):
        rows, expert = args
        gate = jnp.dot(rows, gate_proj[expert], preferred_element_type=jnp.float32)
        up = jnp.dot(rows, up_proj[expert], preferred_element_type=jnp.float32)
        act = (jax.nn.silu(gate) * up).astype(jnp.bfloat16)
        return jnp.dot(act, down_proj[expert], preferred_element_type=jnp.float32).astype(jnp.bfloat16)
    results = lax.map(run_block, (buffer.reshape(block_count, row_block, D), block_expert)).reshape(-1, D)
    contrib = results[dest].astype(jnp.float32) * sorted_weight[:, None]
    return jnp.zeros((TOKEN_COUNT, D), jnp.float32).at[sorted_token].add(contrib)

def reference(query_rows, key_rows, value_rows, forget_cum, doc_ids, residual, out_weight, norm_gain, expert_ids, route_weights, gate_proj, up_proj, down_proj):
    attended = attention(query_rows, key_rows, value_rows, forget_cum, doc_ids)
    mixed = jnp.dot(attended, out_weight, preferred_element_type=jnp.float32)
    hidden = residual.astype(jnp.float32) + mixed
    normed = (hidden * lax.rsqrt(lax.optimization_barrier(jnp.mean(hidden * hidden, axis=-1, keepdims=True)) + norm_eps) * norm_gain).astype(jnp.bfloat16)
    routed = experts_layer(normed, expert_ids, route_weights, gate_proj, up_proj, down_proj)
    return (hidden + routed).astype(jnp.bfloat16)
```

```python
import functools
import math

import jax
import jax.numpy as jnp
from jax import lax
from jax.experimental import pallas as pl
from jax.experimental.pallas import tpu as pltpu
from jax.sharding import PartitionSpec as P

EPG = 4
TOPK = 2
REACH = 3
LOW = -1e30
SHUT = -(2.0**30)

norm_eps = 1e-06


def attend_kernel(
    n,
    parts,
    heads,
    head_size,
    q_ref,
    k_ref,
    v_ref,
    row_ref,
    doc_ref,
    out_ref,
    kb,
    vb,
    mb,
    qa,
    ext,
    rhs,
    vaug,
    acc,
    top_ref,
    stage,
    send_sem,
    recv_sem,
    out_send,
    out_recv,
):
    me = lax.axis_index("sp")
    mine = lax.axis_index("tp")
    odd = lax.rem(me, 2)
    is_odd = odd == 1
    is_even = odd == 0
    partner = me + 1 - 2 * odd
    has_behind = me >= 2
    has_ahead = me < n - 2
    tok, width = q_ref.shape
    pair = 2 * head_size
    pairs = heads // 2
    depth = rhs.shape[1]
    marks = row_ref.shape[0]
    tq = min(256, tok)
    share = tok // parts

    def greet(device):
        pl.semaphore_signal(barrier, inc=1, device_id=device, device_id_type=pl.DeviceIdType.MESH)

    barrier = pltpu.get_barrier_semaphore()
    greet({"sp": partner})

    @pl.when(has_behind)
    def _():
        greet({"sp": me - 2})

    @pl.when(has_ahead)
    def _():
        greet({"sp": me + 2})

    for d in range(1, parts):
        greet({"tp": lax.rem(mine + d, parts)})

    peers = 3 - (me < 2).astype(jnp.int32) - (me >= n - 2).astype(jnp.int32)
    pl.semaphore_wait(barrier, peers + (parts - 1))

    def copies(source, slot, target, c):
        high = pl.ds(c * pair, pair)
        if source is None:
            found = (k_ref.at[high, :], v_ref.at[:, high], row_ref)
        else:
            found = (kb.at[source, high, :], vb.at[source, :, high], mb.at[source])
        into = (kb.at[slot, high, :], vb.at[slot, :, high], mb.at[slot])
        return [
            pltpu.make_async_remote_copy(
                src_ref=found[j],
                dst_ref=into[j],
                send_sem=send_sem.at[slot, c, j],
                recv_sem=recv_sem.at[slot, c, j],
                device_id={"sp": target},
                device_id_type=pl.DeviceIdType.MESH,
            )
            for j in range(3 if c == 0 else 2)
        ]

    def send(source, slot, target, c):
        for copy in copies(source, slot, target, c):
            copy.start()

    def arrived(slot, c):
        for copy in copies(None, slot, partner, c):
            copy.wait_recv()

    def sent(source, slot, target):
        for c in range(pairs):
            for copy in copies(source, slot, target, c):
                copy.wait_send()

    for c in range(pairs):

        @pl.when(has_ahead)
        def _():
            send(None, 0, me + 2, c)

        @pl.when(is_even)
        def _():
            send(None, 1, partner, c)

    origin = row_ref[:, 0:1]
    log2e = math.log2(math.e)
    rooms = depth - pair - 4 * marks

    def extend(rows):
        doc = rows[heads : heads + 1, :]
        rows = (rows - origin) * log2e
        first = rows.astype(jnp.bfloat16).astype(jnp.float32)
        rest = rows - first
        second = rest.astype(jnp.bfloat16).astype(jnp.float32)
        third = rest - second
        hot = lax.broadcasted_iota(jnp.int32, (rooms, tok), 0).astype(jnp.float32) == doc
        ext[...] = jnp.concatenate(
            [first, second, third, jnp.zeros_like(third), hot.astype(jnp.float32)], axis=0
        ).astype(jnp.bfloat16)

    lane = lax.broadcasted_iota(jnp.int32, (tok, pair), 1)
    side = lax.broadcasted_iota(jnp.int32, (tok, depth - pair), 1)
    closed = (side >= 4 * marks) & (side - 4 * marks != doc_ref[...])
    for h in range(heads):
        c, low = h // 2, (h % 2) * head_size
        here = (lane >= low) & (lane < low + head_size)
        query = q_ref[:, c * pair : (c + 1) * pair].astype(jnp.float32) * (log2e * head_size ** (-0.5))
        coarse = query.astype(jnp.bfloat16).astype(jnp.float32)
        fine = pltpu.roll(query - coarse, head_size, 1)
        qa[h, :, 0:pair] = jnp.where(here, coarse, fine).astype(jnp.bfloat16)
        picks = (side == h) | (side == marks + h) | (side == 2 * marks + h)
        qa[h, :, pair:] = jnp.where(picks, -1.0, jnp.where(closed, SHUT, 0.0)).astype(jnp.bfloat16)

    def prepare(keys, values, c):
        for i in range(2):
            low = i * head_size
            here = (lane >= low) & (lane < low + head_size)
            part = keys[c * pair + low : c * pair + low + head_size, :]
            rhs[i, 0:head_size, :] = part
            rhs[i, head_size:pair, :] = part
            rhs[i, pair:, :] = ext[...]
            two = values[:, c * pair : (c + 1) * pair]
            vaug[i] = jnp.where(here, two, jnp.ones_like(two))

    def accumulate(score, h, i, rows, count, own):
        top = jnp.max(score, axis=1, keepdims=True)
        if not own:
            before = top_ref[h, rows, :]
            top = jnp.maximum(before, top)
            factor = jnp.exp2(before - top)
        expo = jnp.exp2(score - top[:, 0:1]).astype(jnp.bfloat16)
        product = jnp.dot(expo, vaug[i, 0:count, :], preferred_element_type=jnp.float32)
        if own:
            acc[h, rows, :] = product
        else:
            acc[h, rows, :] = acc[h, rows, :] * factor + product
        top_ref[h, rows, :] = jnp.broadcast_to(top, (tq, pair))

    def compute_own(c):
        prepare(k_ref, v_ref, c)
        for t in range(tok // tq):
            count = (t + 1) * tq
            rows = slice(t * tq, count)
            for i in range(2):
                h = 2 * c + i
                score = jnp.dot(
                    qa[h, rows, :], rhs[i, :, 0:count], preferred_element_type=jnp.float32
                )
                q_pos = lax.broadcasted_iota(jnp.int32, (tq, count), 0) + t * tq
                k_pos = lax.broadcasted_iota(jnp.int32, (tq, count), 1)
                score = jnp.where(k_pos <= q_pos, score, LOW)
                accumulate(score, h, i, rows, count, True)

    def compute(slot, c):
        prepare(kb.at[slot], vb.at[slot], c)

        def tile(t, carry):
            rows = pl.ds(pl.multiple_of(t * tq, tq), tq)
            for i in range(2):
                h = 2 * c + i
                score = jnp.dot(qa[h, rows, :], rhs[i], preferred_element_type=jnp.float32)
                accumulate(score, h, i, rows, tok, False)
            return carry

        lax.fori_loop(0, tok // tq, tile, 0)

    extend(row_ref[...])
    for c in range(pairs):
        compute_own(c)

    @pl.when(has_behind)
    def _():
        for c in range(pairs):
            arrived(0, c)
            send(0, 2, partner, c)

            @pl.when(is_odd & has_ahead)
            def _():
                send(0, 3, me + 2, c)

            if c == 0:
                extend(mb[0])
            compute(0, c)

    @pl.when(is_odd | has_behind)
    def _():
        slot = 2 - odd
        for c in range(pairs):

            @pl.when(is_odd)
            def _():
                arrived(1, c)

            @pl.when(is_even)
            def _():
                arrived(2, c)

            if c == 0:
                extend(mb[slot])
            compute(slot, c)

    @pl.when((is_odd & has_behind) | (me >= 4))
    def _():
        slot = 4 - 2 * odd
        for c in range(pairs):

            @pl.when(is_odd & (me >= 4))
            def _():
                arrived(3, c)
                send(3, 4, partner, c)

            @pl.when(is_odd)
            def _():
                arrived(2, c)

            @pl.when(is_even)
            def _():
                arrived(4, c)

            if c == 0:
                extend(mb[slot])
            compute(slot, c)

    def hand(j, peer):
        return pltpu.make_async_remote_copy(
            src_ref=stage.at[j],
            dst_ref=out_ref.at[mine],
            send_sem=out_send.at[j],
            recv_sem=out_recv.at[mine],
            device_id={"tp": peer},
            device_id_type=pl.DeviceIdType.MESH,
        )

    def finish(d, carry):
        peer = lax.rem(mine + d, parts)
        rows = pl.ds(pl.multiple_of(peer * share, share), share)
        lane = lax.broadcasted_iota(jnp.int32, (share, pair), 1)
        for c in range(pairs):
            both = []
            for i in range(2):
                found = acc[2 * c + i, rows, :]
                both.append(found / pltpu.roll(found, head_size, 1))
            stage[d, :, c * pair : (c + 1) * pair] = jnp.where(
                lane < head_size, both[0], both[1]
            ).astype(jnp.bfloat16)

        @pl.when(d < parts)
        def _():
            hand(d, peer).start()

        return carry

    lax.fori_loop(1, parts + 1, finish, 0)
    out_ref[mine] = stage[parts]
    for d in range(1, parts):
        other = lax.rem(mine + d, parts)
        pltpu.make_async_remote_copy(
            src_ref=stage.at[d],
            dst_ref=out_ref.at[other],
            send_sem=out_send.at[d],
            recv_sem=out_recv.at[other],
            device_id={"tp": other},
            device_id_type=pl.DeviceIdType.MESH,
        ).wait_recv()
    for d in range(1, parts):
        hand(d, lax.rem(mine + d, parts)).wait_send()

    @pl.when(has_ahead)
    def _():
        sent(None, 0, me + 2)

    @pl.when(is_even)
    def _():
        sent(None, 1, partner)

    @pl.when(has_behind)
    def _():
        sent(0, 2, partner)

    @pl.when(is_odd & has_behind & has_ahead)
    def _():
        sent(0, 3, me + 2)

    @pl.when(is_odd & (me >= 4))
    def _():
        sent(3, 4, partner)


def attention(query_rows, key_rows, value_rows, forget_cum, doc_ids):
    tok, width = query_rows.shape
    heads = forget_cum.shape[0]
    head_size = width // heads
    pair = 2 * head_size
    pairs = heads // 2
    lines = -(-(heads + 1) // 8) * 8
    marks = jnp.concatenate(
        [
            forget_cum,
            doc_ids.astype(jnp.float32)[None],
            jnp.zeros((lines - heads - 1, tok), jnp.float32),
        ]
    )
    n, parts = lax.axis_size("sp"), lax.axis_size("tp")
    share = tok // parts
    depth = 2 * pair
    whole = pl.BlockSpec(memory_space=pltpu.VMEM)
    found = pl.pallas_call(
        functools.partial(attend_kernel, n, parts, heads, head_size),
        out_shape=jax.ShapeDtypeStruct((parts, share, width), jnp.bfloat16),
        in_specs=[whole] * 5,
        out_specs=whole,
        scratch_shapes=[
            pltpu.VMEM((5, width, tok), jnp.bfloat16),
            pltpu.VMEM((5, tok, width), jnp.bfloat16),
            pltpu.VMEM((5, lines, tok), jnp.float32),
            pltpu.VMEM((heads, tok, depth), jnp.bfloat16),
            pltpu.VMEM((depth - pair, tok), jnp.bfloat16),
            pltpu.VMEM((2, depth, tok), jnp.bfloat16),
            pltpu.VMEM((2, tok, pair), jnp.bfloat16),
            pltpu.VMEM((heads, tok, pair), jnp.float32),
            pltpu.VMEM((heads, tok, pair), jnp.float32),
            pltpu.VMEM((parts + 1, share, width), jnp.bfloat16),
            pltpu.SemaphoreType.DMA((5, pairs, 3)),
            pltpu.SemaphoreType.DMA((5, pairs, 3)),
            pltpu.SemaphoreType.DMA((parts,)),
            pltpu.SemaphoreType.DMA((parts,)),
        ],
        compiler_params=pltpu.CompilerParams(collective_id=0, has_side_effects=True),
        cost_estimate=pl.CostEstimate(
            flops=64 * tok * tok * width, bytes_accessed=8 * tok * width, transcendentals=4 * heads * tok * tok
        ),
        name="attend",
    )(query_rows, key_rows.T, value_rows, marks, doc_ids.astype(jnp.int32)[:, None])
    return jnp.transpose(found, (1, 0, 2)).reshape(share, parts * width)


def mirror_piece(gate, up, down):
    n, parts = lax.axis_size("sp"), lax.axis_size("tp")
    part = gate.shape[1] // parts
    first = lax.axis_index("tp") * part
    piece = (
        lax.dynamic_slice_in_dim(gate, first, part, 1),
        lax.dynamic_slice_in_dim(up, first, part, 1),
        lax.dynamic_slice_in_dim(down, first, part, 0),
    )
    piece = (jnp.concatenate(piece[:2], axis=1), piece[2])
    across = [(i, (i + n // 2) % n) for i in range(n)]
    piece = [lax.ppermute(each, "sp", across) for each in piece]
    return piece


def gather_mirror(piece):
    parts = lax.axis_size("tp")
    found = [piece]
    step = parts // 2
    while step > 0:
        route = [(i, i ^ step) for i in range(parts)]
        found = found + [[lax.ppermute(x, "tp", route) for x in each] for each in found]
        step = step // 2
    part = piece[1].shape[0]
    return (
        jnp.concatenate([each[0][:, :part] for each in found], axis=1),
        jnp.concatenate([each[0][:, part:] for each in found], axis=1),
        jnp.concatenate([each[1] for each in found], axis=0),
    )


def per_device(
    query_rows,
    key_rows,
    value_rows,
    forget_cum,
    doc_ids,
    residual,
    out_weight,
    norm_gain,
    expert_ids,
    route_weights,
    gate_proj,
    up_proj,
    down_proj,
):
    piece = mirror_piece(gate_proj[0], up_proj[0], down_proj[0])
    attended = attention(query_rows, key_rows, value_rows, forget_cum, doc_ids)
    attended, piece = lax.optimization_barrier((attended, piece))
    mirror_gate, mirror_up, mirror_down = gather_mirror(piece)
    tok_loc = residual.shape[0]
    mixed = jnp.dot(attended, out_weight, preferred_element_type=jnp.float32)
    hidden = residual.astype(jnp.float32) + mixed
    normed = (
        hidden * lax.rsqrt(jnp.mean(hidden * hidden, axis=-1, keepdims=True) + norm_eps) * norm_gain
    ).astype(jnp.bfloat16)
    experts = lax.axis_size("sp")
    half = experts // 2
    groups = experts // EPG
    capacity = min(tok_loc, 2 * max(2, 5 * tok_loc // (4 * groups)))
    width = normed.shape[1]
    halves = [list(range(half)), list(range(half, experts))]
    flat = expert_ids.reshape(-1)
    target = flat % half
    own = (flat // half == lax.axis_index("sp") // half).astype(jnp.bfloat16)
    onehot = (target[:, None] == jnp.arange(half, dtype=jnp.int32)[None, :]).astype(jnp.int32)
    earlier = jnp.cumsum(onehot, axis=0) - onehot
    slot = target * capacity + jnp.sum(earlier * onehot, axis=1)
    select = (jnp.arange(half * capacity, dtype=jnp.int32)[:, None] == slot[None, :]).astype(
        jnp.bfloat16
    )
    select_tokens = select.reshape(half * capacity, tok_loc, TOPK).sum(axis=-1)
    own_rows = jnp.dot(select, own, preferred_element_type=jnp.float32).reshape(half, capacity)

    def exchange(block):
        return lax.all_to_all(
            block, "sp", split_axis=0, concat_axis=0, axis_index_groups=halves, tiled=True
        )

    own_rows = exchange(own_rows).reshape(-1, 1) > 0.5
    sent = jnp.dot(select_tokens, normed, preferred_element_type=jnp.float32).astype(jnp.bfloat16)
    arrived = exchange(sent.reshape(half, capacity, width))
    rows = arrived.reshape(-1, width)

    def activate(gate_weight, up_weight):
        gate = jnp.dot(rows, gate_weight, preferred_element_type=jnp.float32)
        up = jnp.dot(rows, up_weight, preferred_element_type=jnp.float32)
        return (jax.nn.silu(gate) * up).astype(jnp.bfloat16)

    act_own = jnp.where(own_rows, activate(gate_proj[0], up_proj[0]), 0)
    act_mirror = jnp.where(own_rows, 0, activate(mirror_gate, mirror_up))
    act = jnp.concatenate([act_own, act_mirror], axis=1)
    down = jnp.concatenate([down_proj[0], mirror_down], axis=0)
    outcome = jnp.dot(act, down, preferred_element_type=jnp.float32).astype(jnp.bfloat16)
    back = exchange(outcome.reshape(arrived.shape))
    back_rows = back.reshape(half * capacity, width)
    picked = lax.dot_general(
        select, back_rows, (((0,), (0,)), ((), ())), preferred_element_type=jnp.float32
    )
    picked = picked.reshape(tok_loc, TOPK, width)
    combined = jnp.sum(picked * route_weights[:, :, None], axis=1)
    return (hidden + combined).astype(jnp.bfloat16)


def solution(mesh):
    placed = (
        P("sp", "tp"),
        P("sp", "tp"),
        P("sp", "tp"),
        P("tp", "sp"),
        P("sp"),
        P(("sp", "tp"), None),
        P(),
        P(),
        P(("sp", "tp"), None),
        P(("sp", "tp"), None),
        P("sp", None, None),
        P("sp", None, None),
        P("sp", None, None),
    )
    return jax.shard_map(
        per_device, mesh=mesh, in_specs=placed, out_specs=P(("sp", "tp"), None), check_vma=False
    )
```
